32 devices in a mesh: sp: 8 (over z, y), tp: 4 (over x, core).
Axes of the slice: x: 2, y: 2, z: 4, core: 2. Of those that a mesh axis runs over, the one named last changes fastest.
Arguments:
- out_grad: bfloat16 [1024, 2048], P('sp', 'tp'), may hold values from -6 to 6
- route_ids: int32 [1024, 2], P('sp'), may hold values from 0 to 7, as said below
- route_weight: float32 [1024, 2], P('sp'), may hold values from 0.1 to 0.9
- expert_inputs: bfloat16 [8, 512, 2048], P('sp'), may hold values from -6 to 6
- gate_weight: bfloat16 [8, 2048, 3072], P('sp', None, 'tp'), may hold values from -0.125 to 0.125
- up_weight: bfloat16 [8, 2048, 3072], P('sp', None, 'tp'), may hold values from -0.125 to 0.125
- down_weight: bfloat16 [8, 3072, 2048], P('sp', 'tp'), may hold values from -0.109375 to 0.109375
- out_gate: bfloat16 [1024, 2048], P('sp', 'tp'), may hold values from -6 to 6
- in_gate: bfloat16 [1024, 2048], P('sp', 'tp'), may hold values from -6 to 6
- values: bfloat16 [1024, 2048], P('sp', 'tp'), may hold values from -6 to 6
- conv_out: bfloat16 [1024, 2048], P('sp', 'tp'), may hold values from -6 to 6
- conv_taps: bfloat16 [3, 2048], P(None, 'tp'), may hold values from -3.5 to 3.5
- proj_weight: bfloat16 [2048, 2048], P(None, 'tp'), may hold values from -0.125 to 0.125
Outputs:
- resid_grad: bfloat16 [1024, 2048], P('sp', 'tp')
- out_gate_grad: bfloat16 [1024, 2048], P('sp', 'tp')
- in_gate_grad: bfloat16 [1024, 2048], P('sp', 'tp')
- values_grad: bfloat16 [1024, 2048], P('sp', 'tp')
- proj_grad: float32 [2048, 2048], P('sp', 'tp')
- gate_grad: bfloat16 [8, 2048, 3072], P('sp', None, 'tp')
- up_grad: bfloat16 [8, 2048, 3072], P('sp', None, 'tp')
- down_grad: bfloat16 [8, 3072, 2048], P('sp', 'tp')
The draws below stay inside these ranges and needn't reach their ends.
Inputs may be any that keep to these rules, and one draw needn't show every extreme that they name: `route_ids`: each row names two different experts. Among the rows of one device (aligned blocks of 128 rows) no expert is named more than 64 times, and in every draw one expert is named exactly 64 times in every block.
All inputs are finite; a program needn't handle non-finite values.
Results may differ from the reference program's by a relative error of at most 0.017.
Values may be sent and summed in bfloat16 or wider, within the bound.
A program may use at most 128 MiB of HBM per device.

```python
import math
import jax
import jax.numpy as jnp
from jax import lax

D = 2048
FF = 3072
TAPS = 3
TOK_DEV = 128
TOKENS = 1024
EXPERTS = 8
CAP = 64
SLOTS = 512
N_TP = 4


def draw_route_ids(key, part):
    blocks = TOKENS // TOK_DEV
    tickets = jnp.arange(EXPERTS * CAP, dtype=jnp.int32) // CAP
    filled = jax.random.randint(jax.random.fold_in(key, 11), (), 0, EXPERTS)

    def one_block(block_key):
        extra = jax.random.randint(jax.random.fold_in(block_key, 1), (), 0, EXPERTS)
        shuffled = tickets[jax.random.permutation(jax.random.fold_in(block_key, 2), EXPERTS * CAP)]
        priority = jnp.where(shuffled == filled, 0, jnp.where(shuffled == extra, 1, 2)).astype(jnp.int32)
        chosen = shuffled[jnp.argsort(priority, stable=True)][:2 * TOK_DEV]
        ordered = jnp.sort(chosen)
        pairs = jnp.stack([ordered[:TOK_DEV], ordered[TOK_DEV:]], axis=1)
        flips = jax.random.randint(jax.random.fold_in(block_key, 3), (TOK_DEV, 1), 0, 2)
        pairs = jnp.where(flips == 1, pairs[:, ::-1], pairs)
        shuffle_rows = jax.random.permutation(jax.random.fold_in(block_key, 4), TOK_DEV)
        return pairs[shuffle_rows]
    block_keys = jax.random.split(jax.random.fold_in(key, 7), blocks)
    return jax.vmap(one_block)(block_keys).reshape(TOKENS, 2).astype(jnp.int32)


def spiked(values, key, source, target, blocks, factor):
    def block_of(position):
        return (jnp.arange(values.shape[position]) // (values.shape[position] // blocks)).reshape((-1,) + (1,) * (values.ndim - 1 - position))

    first = jax.random.permutation(key, blocks)[block_of(target)]
    other_side = (block_of(target) + blocks // 2) % blocks
    return jnp.where((block_of(source) == first) | (block_of(source) == other_side), factor * values, values)


def levels(rng, extent, pieces, least, largest):
    level, own = 1.0, jax.random.fold_in(rng, 6)
    for axis_at, parts in pieces:
        heights = jnp.exp(jax.random.uniform(jax.random.fold_in(own, axis_at), (parts,), jnp.float32, least / len(pieces), largest / len(pieces)))
        level = level * jnp.repeat(heights, extent[axis_at] // parts).reshape([-1 if axis == axis_at else 1 for axis in range(len(extent))])
    return level


def centred(own_key, dims, deviation, reach, cuts=(), held_as=jnp.bfloat16):
    level = levels(own_key, dims, cuts, -0.22, 0.18) if cuts else 1.0
    entries = jax.random.normal(own_key, dims, jnp.float32) * deviation * level
    return jnp.minimum(jnp.maximum(entries, -reach), reach).astype(held_as)


def bell_draw_with(own_key, shape, scale, bound, shards, heavy, kind=jnp.bfloat16):
    values = scale * jax.random.normal(own_key, shape, jnp.float32)
    if shards:
        values = values * levels(own_key, shape, shards, -0.22, 0.18)
    return jnp.clip(spiked(values, jax.random.fold_in(own_key, 3), *heavy), -bound, bound).astype(kind)


def setup_inputs(seed: int = 0) -> dict:
    streams_of = jax.random.split(jax.random.key(seed), 14)
    out_grad = bell_draw_with(streams_of[0], (TOKENS, D), 1.0, 6.0, ((0, 8), (1, 4)), (0, 1, 8, 2.0))
    route_ids = draw_route_ids(jax.random.fold_in(streams_of[13], 71), 0)
    route_weight = jnp.clip(0.1 + 0.79999997 * jax.random.uniform(streams_of[2], (TOKENS, 2), jnp.float32) ** levels(streams_of[2], (TOKENS, 2), ((0, 8),), -0.2, 0.2), 0.1, 0.9)
    expert_inputs = centred(streams_of[3], (EXPERTS, SLOTS, D), 1.0, 6.0, ((0, 8),))
    gate_weight = centred(streams_of[4], (EXPERTS, D, FF), D ** -0.5, 0.125, ((0, 8), (2, 4)))
    up_weight = centred(streams_of[5], (EXPERTS, D, FF), D ** -0.5, 0.125, ((0, 8), (2, 4)))
    down_weight = centred(streams_of[6], (EXPERTS, FF, D), FF ** -0.5, 0.109375, ((0, 8), (1, 4)))
    out_gate = centred(streams_of[7], (TOKENS, D), 1.0, 6.0, ((0, 8), (1, 4)))
    in_gate = centred(streams_of[8], (TOKENS, D), 1.0, 6.0, ((0, 8), (1, 4)))
    values = centred(streams_of[9], (TOKENS, D), 1.0, 6.0, ((0, 8), (1, 4)))
    conv_out = centred(streams_of[10], (TOKENS, D), 1.0, 6.0, ((0, 8), (1, 4)))
    conv_taps = centred(streams_of[11], (TAPS, D), TAPS ** -0.5, 3.5, ((1, 4),))
    proj_weight = centred(streams_of[12], (D, D), D ** -0.5, 0.125, ((1, 4),))
    return dict(out_grad=out_grad, route_ids=route_ids, route_weight=route_weight, expert_inputs=expert_inputs, gate_weight=gate_weight, up_weight=up_weight, down_weight=down_weight, out_gate=out_gate, in_gate=in_gate, values=values, conv_out=conv_out, conv_taps=conv_taps, proj_weight=proj_weight)


def slot_rows(route_ids):
    blocks = route_ids.reshape(TOKENS // TOK_DEV, 2 * TOK_DEV)
    onehot = (blocks[:, :, None] == jnp.arange(EXPERTS, dtype=jnp.int32)[None, None, :]).astype(jnp.int32)
    ranked = lax.optimization_barrier(jnp.sum((jnp.cumsum(onehot, axis=1) - onehot) * onehot, axis=2))
    source = jnp.arange(TOKENS // TOK_DEV, dtype=jnp.int32)[:, None]
    return (blocks * SLOTS + source * CAP + ranked).reshape(-1).astype(jnp.int32)

def expert_step(operands):
    inputs, routed, gate_w, up_w, down_w = operands
    pre_gate = jnp.dot(inputs, gate_w, preferred_element_type=jnp.float32)
    pre_up = jnp.dot(inputs, up_w, preferred_element_type=jnp.float32)
    sigmoid_g = jax.nn.sigmoid(pre_gate)
    activated = pre_gate * sigmoid_g
    hidden = (activated * pre_up).astype(jnp.bfloat16)
    d_hidden = jnp.dot(routed, down_w.T, preferred_element_type=jnp.float32)
    d_gate = (d_hidden * pre_up * sigmoid_g * (1.0 + pre_gate * (1.0 - sigmoid_g))).astype(jnp.bfloat16)
    d_up = (d_hidden * activated).astype(jnp.bfloat16)
    slot_scale = 1.0 / math.sqrt(SLOTS)
    gate_grad = (jnp.dot(inputs.T, d_gate, preferred_element_type=jnp.float32) * slot_scale).astype(jnp.bfloat16)
    up_grad = (jnp.dot(inputs.T, d_up, preferred_element_type=jnp.float32) * slot_scale).astype(jnp.bfloat16)
    down_grad = (jnp.dot(hidden.T, routed, preferred_element_type=jnp.float32) * slot_scale).astype(jnp.bfloat16)
    block_width = FF // N_TP
    back = jnp.zeros((SLOTS, D), jnp.float32)
    for block in range(N_TP):
        lower = block * block_width
        upper = lower + block_width
        part_sum = jnp.dot(lax.slice_in_dim(d_gate, lower, upper, axis=1), lax.slice_in_dim(gate_w, lower, upper, axis=1).T, preferred_element_type=jnp.float32)
        part_sum = part_sum + jnp.dot(lax.slice_in_dim(d_up, lower, upper, axis=1), lax.slice_in_dim(up_w, lower, upper, axis=1).T, preferred_element_type=jnp.float32)
        back = back + lax.optimization_barrier(part_sum.astype(jnp.bfloat16)).astype(jnp.float32)
    return (gate_grad, up_grad, down_grad, back.astype(jnp.bfloat16))

def reference(out_grad, route_ids, route_weight, expert_inputs, gate_weight, up_weight, down_weight, out_gate, in_gate, values, conv_out, conv_taps, proj_weight):
    rows = slot_rows(route_ids)
    weighted = (route_weight[:, :, None] * out_grad.astype(jnp.float32)[:, None, :]).astype(jnp.bfloat16).reshape(2 * TOKENS, D)
    routed = jnp.zeros((EXPERTS * SLOTS, D), jnp.bfloat16).at[rows].set(weighted).reshape(EXPERTS, SLOTS, D)
    gate_grad, up_grad, down_grad, back = lax.map(expert_step, (expert_inputs, routed, gate_weight, up_weight, down_weight))
    pair_back = back.reshape(EXPERTS * SLOTS, D)[rows].astype(jnp.float32).reshape(TOKENS, 2, D)
    resid_grad = (out_grad.astype(jnp.float32) + pair_back[:, 0] + pair_back[:, 1]).astype(jnp.bfloat16)
    gate_vals = out_gate.astype(jnp.float32)
    conv_vals = conv_out.astype(jnp.float32)
    mixed_in = (gate_vals * conv_vals).astype(jnp.bfloat16)
    proj_grad = jnp.dot(resid_grad.T, mixed_in, preferred_element_type=jnp.float32) * (1.0 / math.sqrt(TOKENS))
    mix_grad = jnp.dot(resid_grad, proj_weight, preferred_element_type=jnp.float32)
    out_gate_grad = (mix_grad * conv_vals).astype(jnp.bfloat16)
    conv_grad = lax.optimization_barrier((mix_grad * gate_vals).astype(jnp.bfloat16)).astype(jnp.float32)
    padded = jnp.pad(conv_grad, ((1, 1), (0, 0)))
    tap_vals = conv_taps.astype(jnp.float32)
    value_grad = padded[2:] * tap_vals[0] + padded[1:-1] * tap_vals[1] + padded[:-2] * tap_vals[2]
    in_gate_grad = (value_grad * values.astype(jnp.float32)).astype(jnp.bfloat16)
    values_grad = (value_grad * in_gate.astype(jnp.float32)).astype(jnp.bfloat16)
    return (resid_grad, out_gate_grad, in_gate_grad, values_grad, proj_grad, gate_grad, up_grad, down_grad)
```

```python
import functools
import math

import jax
import jax.numpy as jnp
from jax import lax
from jax.experimental import pallas as pl
from jax.experimental.pallas import tpu as pltpu
from jax.sharding import PartitionSpec as P

BF = jnp.bfloat16
F32 = jnp.float32
MESH = pl.DeviceIdType.MESH
VMEM = pl.BlockSpec(memory_space=pltpu.VMEM)
ANY = pl.BlockSpec(memory_space=pl.ANY)


def dot(left, right, dims):
    return lax.dot_general(left, right, ((dims[0], dims[1]), ((), ())), preferred_element_type=F32)


def remote(src, dst, send, recv, device):
    return pltpu.make_async_remote_copy(
        src_ref=src, dst_ref=dst, send_sem=send, recv_sem=recv, device_id=device, device_id_type=MESH
    )


def greet(n_sp, me, partners):
    barrier = pltpu.get_barrier_semaphore()
    for d in range(1, n_sp):
        pl.semaphore_signal(
            barrier, inc=1, device_id={"sp": lax.rem(me + d, n_sp)}, device_id_type=MESH
        )
    for tp in partners:
        pl.semaphore_signal(barrier, inc=1, device_id={"tp": tp}, device_id_type=MESH)
    pl.semaphore_wait(barrier, n_sp - 1 + len(partners))


class Exchange:
    def __init__(self, n_sp, me, tp, sib, far, src_at, dst_at, sems):
        self.n_sp, self.me, self.tp, self.sib, self.far = n_sp, me, tp, sib, far
        self.src_at, self.dst_at, self.sems = src_at, dst_at, sems

    def source(self, d):
        return lax.rem(self.me - d + self.n_sp, self.n_sp)

    def sp_copy(self, d):
        to = lax.rem(self.me + d, self.n_sp)
        return remote(
            self.src_at(to), self.dst_at(self.tp, self.me),
            self.sems.at[0, d], self.sems.at[1, d], {"sp": to},
        )

    def far_copy(self, d):
        place = self.dst_at(self.tp, self.source(d))
        return remote(place, place, self.sems.at[2, d], self.sems.at[3, d], {"tp": self.far})

    def sib_copy(self, d):
        place = self.dst_at(self.tp, self.source(d))
        return remote(place, place, self.sems.at[4, d], self.sems.at[5, d], {"tp": self.sib})

    def hand_copy(self, d):
        place = self.dst_at(self.far, self.source(d))
        return remote(place, place, self.sems.at[6, d], self.sems.at[7, d], {"tp": self.sib})

    def start(self):
        for d in range(1, self.n_sp):
            self.sp_copy(d).start()
        own = pltpu.make_async_copy(
            self.src_at(self.me), self.dst_at(self.tp, self.me), self.sems.at[0, 0]
        )
        own.start()
        own.wait()
        self.far_copy(0).start()
        self.sib_copy(0).start()

    def step(self, d):
        self.sp_copy(d).wait_recv()
        self.far_copy(d).start()
        self.sib_copy(d).start()
        self.far_copy(d - 1).wait_recv()
        self.hand_copy(d - 1).start()

    def steps(self, first, last):
        @pl.loop(first, last)
        def _(d):
            self.step(d)

    def finish(self):
        n = self.n_sp
        self.far_copy(n - 1).wait_recv()
        self.hand_copy(n - 1).start()

        @pl.loop(0, n)
        def _(d):
            self.far_copy(d).wait_send()
            self.sib_copy(d).wait_send()
            self.sib_copy(d).wait_recv()
            self.hand_copy(d).wait_send()
            self.hand_copy(d).wait_recv()

        @pl.loop(1, n)
        def _(d):
            self.sp_copy(d).wait_send()


def expert_kernel(
    n_sp, n_tp, experts,
    og_ref, ids_ref, rw_ref, x_hbm, gw_hbm, uw_hbm, dw_hbm,
    routed, hidden, dall, resid, rfull, quarter,
    x, w, dw, pre, outgoing, parts, from_sib, far_out, far_in, total, final, back, disp,
    load_sems, ex_sems, sib_sems, far_sems, ret_sems, gat_sems,
):
    me, tp = lax.axis_index("sp"), lax.axis_index("tp")
    sib = tp + 1 - 2 * lax.rem(tp, 2)
    far = lax.rem(tp + n_tp // 2, n_tp)
    tokens, chan = og_ref.shape
    slots, width = x.shape
    hid = dw.shape[0]
    cap = slots // n_sp
    local = experts // n_sp

    loads = [
        pltpu.make_async_copy(x_hbm.at[0], x, load_sems.at[0]),
        pltpu.make_async_copy(gw_hbm.at[0], w.at[:, pl.ds(0, hid)], load_sems.at[1]),
        pltpu.make_async_copy(uw_hbm.at[0], w.at[:, pl.ds(hid, hid)], load_sems.at[2]),
        pltpu.make_async_copy(dw_hbm.at[0], dw, load_sems.at[3]),
    ]
    for load in loads:
        load.start()

    ids = ids_ref[...]
    id0, id1 = ids[:, 0:1], ids[:, 1:2]
    rw = rw_ref[...]
    lanes = lax.broadcasted_iota(jnp.int32, (tokens, 128), 1)
    hit0 = jnp.where(id0 == lanes, 1.0, 0.0).astype(F32)
    hit1 = jnp.where(id1 == lanes, 1.0, 0.0).astype(F32)
    rows = lax.broadcasted_iota(jnp.int32, (tokens, tokens), 0)
    cols = lax.broadcasted_iota(jnp.int32, (tokens, tokens), 1)
    earlier = jnp.where(rows > cols, 1.0, 0.0).astype(BF)
    counts = dot(earlier, (hit0 + hit1).astype(BF), ((1,), (0,)))
    rank0 = jnp.sum(counts * hit0, axis=1, keepdims=True)
    rank1 = jnp.sum(counts * hit1, axis=1, keepdims=True)
    slot0 = id0.astype(F32) * float(cap) + rank0
    slot1 = id1.astype(F32) * float(cap) + rank1
    places = lax.broadcasted_iota(jnp.int32, (tokens, experts * cap), 1).astype(F32)
    d0 = jnp.where(slot0 == places, 1.0, 0.0).astype(BF)
    d1 = jnp.where(slot1 == places, 1.0, 0.0).astype(BF)
    disp[...] = d0 + d1
    og = og_ref[...].astype(F32)
    sent = dot(d0, (rw[:, 0:1] * og).astype(BF), ((0,), (0,)))
    sent = sent + dot(d1, (rw[:, 1:2] * og).astype(BF), ((0,), (0,)))
    outgoing[...] = sent.astype(BF)

    greet(n_sp, me, (sib, far))
    ex = Exchange(
        n_sp, me, tp, sib, far,
        lambda k: outgoing.at[pl.ds(pl.multiple_of(k * cap, cap), cap), :],
        lambda j, s: routed.at[
            pl.ds(pl.multiple_of(s * cap, cap), cap), pl.ds(pl.multiple_of(j * chan, chan), chan)
        ],
        ex_sems,
    )
    ex.start()
    for load in loads:
        load.wait()
    tile = 256
    pre_tiles = 2 * hid // tile
    both = min(pre_tiles, n_sp - 1)

    def pre_dot(t):
        at = pl.ds(pl.multiple_of(t * tile, tile), tile)
        pre[:, at] = dot(x[...], w[:, at], ((1,), (0,)))

    @pl.loop(0, both)
    def _(t):
        ex.step(t + 1)
        pre_dot(t)

    if both < pre_tiles:
        pl.loop(both, pre_tiles)(pre_dot)
    if both < n_sp - 1:
        ex.steps(both + 1, n_sp)
    ex.finish()

    @pl.loop(0, hid // tile)
    def _(t):
        at = pl.ds(pl.multiple_of(t * tile, tile), tile)
        up_at = pl.ds(pl.multiple_of(hid + t * tile, tile), tile)
        d_hidden = dot(routed[...], dw[at, :], ((1,), (1,)))
        gate, up = pre[:, at], pre[:, up_at]
        sig = jax.nn.sigmoid(gate)
        act = gate * sig
        hidden[:, at] = (act * up).astype(BF)
        dall[:, at] = (d_hidden * up * sig * (1.0 + gate * (1.0 - sig))).astype(BF)
        dall[:, up_at] = (d_hidden * act).astype(BF)

    def back_part(block, place):
        @pl.loop(0, chan // tile)
        def _(t):
            at = pl.ds(pl.multiple_of(block * chan + t * tile, tile), tile)
            value = dot(dall[...], w[at, :], ((1,), (1,)))
            parts[place, :, pl.ds(pl.multiple_of(t * tile, tile), tile)] = value.astype(BF)

    far_sib = lax.rem(sib + n_tp // 2, n_tp)
    sib_copies = [
        remote(parts.at[2 * i], from_sib.at[i], sib_sems.at[0, i], sib_sems.at[1, i], {"tp": sib})
        for i in range(2)
    ]

    def at_rows(d):
        s = lax.rem(me + d, n_sp)
        return pl.ds(pl.multiple_of(s * cap, cap), cap)

    def far_copy(d):
        return remote(
            far_out.at[at_rows(d), :], far_in.at[at_rows(d), :],
            far_sems.at[0, lax.rem(d, n_sp)], far_sems.at[1, lax.rem(d, n_sp)], {"tp": far},
        )

    def ret_copy(d):
        mine = pl.ds(pl.multiple_of(me * cap, cap), cap)
        return remote(
            final.at[at_rows(d), :], back.at[mine, :],
            ret_sems.at[0, d], ret_sems.at[1, d], {"sp": lax.rem(me + d, n_sp)},
        )

    back_part(far_sib, 0)
    sib_copies[0].start()
    back_part(far, 1)
    sib_copies[0].wait_recv()

    @pl.loop(1, n_sp + 1)
    def _(d):
        at = at_rows(d)
        far_out[at, :] = (parts[1, at, :].astype(F32) + from_sib[0, at, :].astype(F32)).astype(BF)
        far_copy(d).start()

    back_part(sib, 2)
    sib_copies[1].start()
    back_part(tp, 3)
    sib_copies[1].wait_recv()
    total[...] = parts[3].astype(F32) + from_sib[1].astype(F32)

    @pl.loop(1, n_sp)
    def _(d):
        at = at_rows(d)
        far_copy(d).wait_recv()
        final[at, :] = (total[at, :] + far_in[at, :].astype(F32)).astype(BF)
        ret_copy(d).start()

    far_copy(n_sp).wait_recv()
    at = at_rows(0)
    back[at, :] = (total[at, :] + far_in[at, :].astype(F32)).astype(BF)

    @pl.loop(1, n_sp)
    def _(d):
        ret_copy(d).wait_recv()

    value = (og_ref[...].astype(F32) + dot(disp[...], back[...], ((1,), (0,)))).astype(BF)
    resid[...] = value
    rfull[tp] = value
    near = remote(rfull.at[tp], rfull.at[tp], gat_sems.at[0], gat_sems.at[1], {"tp": sib})
    away = remote(rfull.at[tp], rfull.at[tp], gat_sems.at[2], gat_sems.at[3], {"tp": far})
    away.start()
    near.start()
    away.wait_recv()
    hand = remote(rfull.at[far], rfull.at[far], gat_sems.at[4], gat_sems.at[5], {"tp": sib})
    hand.start()
    near.wait_recv()
    hand.wait_recv()
    share = tokens // n_tp
    piece = width // n_sp
    for k in range(n_sp):
        block, first = divmod(k * piece, chan)
        quarter[k] = rfull[
            block, pl.ds(pl.multiple_of(tp * share, share), share), first:first + piece
        ]
    near.wait_send()
    away.wait_send()
    hand.wait_send()
    for copy in sib_copies:
        copy.wait_send()

    @pl.loop(1, n_sp)
    def _(d):
        far_copy(d).wait_send()
        ret_copy(d).wait_send()

    far_copy(n_sp).wait_send()


def mixer_kernel(
    n_sp, n_tp,
    quarter, rfull, pw_hbm, og_ref, ig_ref, val_ref, conv_ref, taps_ref,
    columns, og_out, ig_out, val_out,
    pw, edge_out, edge_in, ex_sems, halo_sems, load_sem,
):
    me, tp = lax.axis_index("sp"), lax.axis_index("tp")
    sib = tp + 1 - 2 * lax.rem(tp, 2)
    far = lax.rem(tp + n_tp // 2, n_tp)
    tokens, chan = og_ref.shape
    load = pltpu.make_async_copy(pw_hbm, pw, load_sem)
    load.start()
    greet(n_sp, me, (sib, far))
    ex = Exchange(
        n_sp, me, tp, sib, far, lambda k: quarter.at[k], lambda j, s: columns.at[s, j], ex_sems
    )
    ex.start()
    load.wait()
    mix = dot(rfull[0], pw[0:chan, :], ((1,), (0,)))
    for j in range(1, n_tp):
        mix = mix + dot(rfull[j], pw[j * chan:(j + 1) * chan, :], ((1,), (0,)))
    og_out[...] = (mix * conv_ref[...].astype(F32)).astype(BF)
    grad = (mix * og_ref[...].astype(F32)).astype(BF).astype(F32)
    edge_out[0] = jnp.broadcast_to(grad[tokens - 1:tokens, :], edge_out.shape[1:])
    edge_out[1] = jnp.broadcast_to(grad[0:1, :], edge_out.shape[1:])
    sides = [lax.rem(me + 1, n_sp), lax.rem(me + n_sp - 1, n_sp)]
    halos = [
        remote(edge_out.at[i], edge_in.at[i], halo_sems.at[0, i], halo_sems.at[1, i], {"sp": sides[i]})
        for i in range(2)
    ]
    for halo in halos:
        halo.start()
    ex.steps(1, n_sp)
    for halo in halos:
        halo.wait()
    before = jnp.where(me == 0, 0.0, edge_in[0, 0:1, :])
    after = jnp.where(me == n_sp - 1, 0.0, edge_in[1, 0:1, :])
    row = lax.broadcasted_iota(jnp.int32, (tokens, chan), 0)
    prev = jnp.where(row == 0, before, pltpu.roll(grad, 1, 0))
    following = jnp.where(row == tokens - 1, after, pltpu.roll(grad, tokens - 1, 0))
    taps = taps_ref[...].astype(F32)
    value_grad = following * taps[0:1, :] + grad * taps[1:2, :] + prev * taps[2:3, :]
    ig_out[...] = (value_grad * val_ref[...].astype(F32)).astype(BF)
    val_out[...] = (value_grad * ig_ref[...].astype(F32)).astype(BF)
    ex.finish()


def in_grads(scale, x, d, gate, up):
    hid = gate.shape[-1]
    left = x[0].T
    gate[0] = (dot(left, d[:, :hid], ((1,), (0,))) * scale).astype(BF)
    up[0] = (dot(left, d[:, hid:], ((1,), (0,))) * scale).astype(BF)


def out_grads(scale, h, r, down):
    down[0] = (dot(h[...].T, r[...], ((1,), (0,))) * scale).astype(BF)


def per_device(
    out_grad, route_ids, route_weight, expert_inputs, gate_weight, up_weight, down_weight,
    out_gate, in_gate, values, conv_out, conv_taps, proj_weight,
):
    n_sp, n_tp = lax.axis_size("sp"), lax.axis_size("tp")
    tokens, chan = out_grad.shape
    local, slots, width = expert_inputs.shape
    hid = gate_weight.shape[2]
    assert local == 1 and n_tp == 4
    share, piece = tokens // n_tp, width // n_sp
    dma = pltpu.SemaphoreType.DMA
    mixed_in = (out_gate.astype(F32) * conv_out.astype(F32)).astype(BF)
    mixed_all = lax.all_gather(mixed_in, "sp", axis=0, tiled=True)

    routed, hidden, dall, resid, rfull, quarter = pl.pallas_call(
        functools.partial(expert_kernel, n_sp, n_tp, n_sp * local),
        out_shape=[
            jax.ShapeDtypeStruct((slots, width), BF),
            jax.ShapeDtypeStruct((slots, hid), BF),
            jax.ShapeDtypeStruct((slots, 2 * hid), BF),
            jax.ShapeDtypeStruct((tokens, chan), BF),
            jax.ShapeDtypeStruct((n_tp, tokens, chan), BF),
            jax.ShapeDtypeStruct((n_sp, share, piece), BF),
        ],
        in_specs=[VMEM] * 3 + [ANY] * 4,
        out_specs=[VMEM] * 6,
        scratch_shapes=[
            pltpu.VMEM((slots, width), BF),
            pltpu.VMEM((width, 2 * hid), BF),
            pltpu.VMEM((hid, width), BF),
            pltpu.VMEM((slots, 2 * hid), F32),
            pltpu.VMEM((slots, chan), BF),
            pltpu.VMEM((4, slots, chan), BF),
            pltpu.VMEM((2, slots, chan), BF),
            pltpu.VMEM((slots, chan), BF),
            pltpu.VMEM((slots, chan), BF),
            pltpu.VMEM((slots, chan), F32),
            pltpu.VMEM((slots, chan), BF),
            pltpu.VMEM((slots, chan), BF),
            pltpu.VMEM((tokens, slots), BF),
            dma((4,)), dma((8, n_sp)), dma((2, 2)), dma((2, n_sp)), dma((2, n_sp)), dma((6,)),
        ],
        compiler_params=pltpu.CompilerParams(
            collective_id=0, has_side_effects=True, vmem_limit_bytes=48 * 2**20
        ),
        name="experts",
    )(out_grad, route_ids, route_weight, expert_inputs, gate_weight, up_weight, down_weight)

    columns, out_gate_grad, in_gate_grad, values_grad = pl.pallas_call(
        functools.partial(mixer_kernel, n_sp, n_tp),
        out_shape=[
            jax.ShapeDtypeStruct((n_sp, n_tp, share, piece), BF),
            jax.ShapeDtypeStruct((tokens, chan), BF),
            jax.ShapeDtypeStruct((tokens, chan), BF),
            jax.ShapeDtypeStruct((tokens, chan), BF),
        ],
        in_specs=[VMEM, VMEM, ANY] + [VMEM] * 5,
        out_specs=[VMEM] * 4,
        scratch_shapes=[
            pltpu.VMEM(proj_weight.shape, BF),
            pltpu.VMEM((2, 8, chan), F32),
            pltpu.VMEM((2, 8, chan), F32),
            dma((8, n_sp)), dma((2, 2)), dma,
        ],
        compiler_params=pltpu.CompilerParams(
            collective_id=1, has_side_effects=True, vmem_limit_bytes=32 * 2**20
        ),
        name="mixer",
    )(quarter, rfull, proj_weight, out_gate, in_gate, values, conv_out, conv_taps)

    slot_scale = 1.0 / math.sqrt(slots)
    wide = 256
    gate_grad, up_grad = pl.pallas_call(
        functools.partial(in_grads, slot_scale),
        grid=(width // wide,),
        in_specs=[
            pl.BlockSpec((1, slots, wide), lambda i: (0, 0, i)),
            pl.BlockSpec((slots, 2 * hid), lambda i: (0, 0)),
        ],
        out_specs=[pl.BlockSpec((1, wide, hid), lambda i: (0, i, 0))] * 2,
        out_shape=[jax.ShapeDtypeStruct((1, width, hid), BF)] * 2,
        name="in_grads",
    )(expert_inputs, dall)
    down_grad = pl.pallas_call(
        functools.partial(out_grads, slot_scale),
        grid=(hid // 256,),
        in_specs=[
            pl.BlockSpec((slots, 256), lambda i: (0, i)),
            pl.BlockSpec((slots, width), lambda i: (0, 0)),
        ],
        out_specs=pl.BlockSpec((1, 256, width), lambda i: (0, i, 0)),
        out_shape=jax.ShapeDtypeStruct((1, hid, width), BF),
        name="out_grads",
    )(hidden, routed)
    proj_sum = lax.dot_general(
        columns.reshape(n_sp * tokens, piece), mixed_all,
        (((0,), (0,)), ((), ())), preferred_element_type=F32,
    )
    proj_grad = proj_sum * (1.0 / math.sqrt(tokens * n_sp))
    return (
        resid, out_gate_grad, in_gate_grad, values_grad, proj_grad, gate_grad, up_grad, down_grad,
    )


def solution(mesh):
    rows = P("sp", "tp")
    in_specs = (
        rows, P("sp", None), P("sp", None), P("sp", None, None), P("sp", None, "tp"),
        P("sp", None, "tp"), P("sp", "tp", None), rows, rows, rows, rows, P(None, "tp"), P(None, "tp"),
    )
    out_specs = (
        rows, rows, rows, rows, rows, P("sp", None, "tp"), P("sp", None, "tp"), P("sp", "tp", None),
    )
    return jax.shard_map(
        per_device, mesh=mesh, in_specs=in_specs, out_specs=out_specs, check_vma=False
    )
```

```python
import functools
import math

import jax
import jax.numpy as jnp
from jax import lax
from jax.experimental import pallas as pl
from jax.experimental.pallas import tpu as pltpu
from jax.sharding import PartitionSpec as P

BF = jnp.bfloat16
F32 = jnp.float32
MESH = pl.DeviceIdType.MESH
VMEM = pl.BlockSpec(memory_space=pltpu.VMEM)
ANY = pl.BlockSpec(memory_space=pl.ANY)


def dot(left, right, dims):
    return lax.dot_general(left, right, ((dims[0], dims[1]), ((), ())), preferred_element_type=F32)


def remote(src, dst, send, recv, device):
    return pltpu.make_async_remote_copy(
        src_ref=src, dst_ref=dst, send_sem=send, recv_sem=recv, device_id=device, device_id_type=MESH
    )


def hail(n_sp, me, partners):
    barrier = pltpu.get_barrier_semaphore()
    for d in range(1, n_sp):
        pl.semaphore_signal(
            barrier, inc=1, device_id={"sp": lax.rem(me + d, n_sp)}, device_id_type=MESH
        )
    for tp in partners:
        pl.semaphore_signal(barrier, inc=1, device_id={"tp": tp}, device_id_type=MESH)


def met(n_sp, partners):
    pl.semaphore_wait(pltpu.get_barrier_semaphore(), n_sp - 1 + len(partners))


class Exchange:
    def __init__(self, n_sp, me, tp, sib, far, src_at, dst_at, sems):
        self.n_sp, self.me, self.tp, self.sib, self.far = n_sp, me, tp, sib, far
        self.src_at, self.dst_at, self.sems = src_at, dst_at, sems

    def source(self, d):
        return lax.rem(self.me - d + self.n_sp, self.n_sp)

    def sp_copy(self, d):
        to = lax.rem(self.me + d, self.n_sp)
        return remote(
            self.src_at(to), self.dst_at(self.tp, self.me),
            self.sems.at[0, d], self.sems.at[1, d], {"sp": to},
        )

    def far_copy(self, d):
        place = self.dst_at(self.tp, self.source(d))
        return remote(place, place, self.sems.at[2, d], self.sems.at[3, d], {"tp": self.far})

    def sib_copy(self, d):
        place = self.dst_at(self.tp, self.source(d))
        return remote(place, place, self.sems.at[4, d], self.sems.at[5, d], {"tp": self.sib})

    def hand_copy(self, d):
        place = self.dst_at(self.far, self.source(d))
        return remote(place, place, self.sems.at[6, d], self.sems.at[7, d], {"tp": self.sib})

    def start(self):
        for d in range(1, self.n_sp):
            self.sp_copy(d).start()
        own = pltpu.make_async_copy(
            self.src_at(self.me), self.dst_at(self.tp, self.me), self.sems.at[0, 0]
        )
        own.start()
        own.wait()
        self.far_copy(0).start()
        self.sib_copy(0).start()

    def spread(self, d):
        self.sp_copy(d).wait_recv()
        self.far_copy(d).start()
        self.sib_copy(d).start()

    def hand(self, d):
        self.far_copy(d).wait_recv()
        self.hand_copy(d).start()

    def finish(self):
        n = self.n_sp

        @pl.loop(0, n)
        def _(d):
            self.far_copy(d).wait_send()
            self.sib_copy(d).wait_send()
            self.sib_copy(d).wait_recv()
            self.hand_copy(d).wait_send()
            self.hand_copy(d).wait_recv()

        @pl.loop(1, n)
        def _(d):
            self.sp_copy(d).wait_send()


def expert_kernel(
    n_sp, n_tp, experts,
    og_ref, ids_ref, rw_ref, x_hbm, gw_hbm, uw_hbm, dw_hbm,
    routed, hidden, dall, resid, rfull, quarter,
    x, w, dw, pre, outgoing, parts, from_sib, far_out, far_in, total, final, back, disp,
    load_sems, ex_sems, sib_sems, far_sems, ret_sems, gat_sems,
):
    me, tp = lax.axis_index("sp"), lax.axis_index("tp")
    sib = tp + 1 - 2 * lax.rem(tp, 2)
    far = lax.rem(tp + n_tp // 2, n_tp)
    tokens, chan = og_ref.shape
    slots, width = x.shape
    hid = dw.shape[0]
    cap = slots // n_sp
    local = experts // n_sp

    loads = [
        pltpu.make_async_copy(x_hbm.at[0], x, load_sems.at[0]),
        pltpu.make_async_copy(gw_hbm.at[0], w.at[:, pl.ds(0, hid)], load_sems.at[1]),
        pltpu.make_async_copy(uw_hbm.at[0], w.at[:, pl.ds(hid, hid)], load_sems.at[2]),
        pltpu.make_async_copy(dw_hbm.at[0], dw, load_sems.at[3]),
    ]
    for load in loads:
        load.start()

    hail(n_sp, me, (sib, far))
    ids = ids_ref[...]
    id0, id1 = ids[:, 0:1], ids[:, 1:2]
    rw = rw_ref[...]
    lanes = lax.broadcasted_iota(jnp.int32, (tokens, 128), 1)
    hit0 = jnp.where(id0 == lanes, 1.0, 0.0).astype(F32)
    hit1 = jnp.where(id1 == lanes, 1.0, 0.0).astype(F32)
    rows = lax.broadcasted_iota(jnp.int32, (tokens, tokens), 0)
    cols = lax.broadcasted_iota(jnp.int32, (tokens, tokens), 1)
    earlier = jnp.where(rows > cols, 1.0, 0.0).astype(BF)
    counts = dot(earlier, (hit0 + hit1).astype(BF), ((1,), (0,)))
    rank0 = jnp.sum(counts * hit0, axis=1, keepdims=True)
    rank1 = jnp.sum(counts * hit1, axis=1, keepdims=True)
    slot0 = id0.astype(F32) * float(cap) + rank0
    slot1 = id1.astype(F32) * float(cap) + rank1
    places = lax.broadcasted_iota(jnp.int32, (tokens, experts * cap), 1).astype(F32)
    d0 = jnp.where(slot0 == places, 1.0, 0.0).astype(BF)
    d1 = jnp.where(slot1 == places, 1.0, 0.0).astype(BF)
    disp[...] = d0 + d1
    og = og_ref[...].astype(F32)
    sent = dot(d0, (rw[:, 0:1] * og).astype(BF), ((0,), (0,)))
    sent = sent + dot(d1, (rw[:, 1:2] * og).astype(BF), ((0,), (0,)))
    outgoing[...] = sent.astype(BF)

    met(n_sp, (sib, far))
    ex = Exchange(
        n_sp, me, tp, sib, far,
        lambda k: outgoing.at[pl.ds(pl.multiple_of(k * cap, cap), cap), :],
        lambda j, s: routed.at[
            pl.ds(pl.multiple_of(s * cap, cap), cap), pl.ds(pl.multiple_of(j * chan, chan), chan)
        ],
        ex_sems,
    )
    ex.start()
    for load in loads:
        load.wait()
    tile = 256
    pre_tiles = 2 * hid // tile
    both = min(pre_tiles, n_sp - 1)

    def pre_dot(t):
        at = pl.ds(pl.multiple_of(t * tile, tile), tile)
        pre[:, at] = dot(x[...], w[:, at], ((1,), (0,)))

    @pl.loop(0, both)
    def _(t):
        ex.spread(t + 1)
        pre_dot(t)
        ex.hand(t)

    if both < pre_tiles:
        pl.loop(both, pre_tiles)(pre_dot)
    if both < n_sp - 1:
        pl.loop(both + 1, n_sp)(ex.spread)
    pl.loop(both, n_sp)(ex.hand)
    ex.finish()

    @pl.loop(0, hid // tile)
    def _(t):
        at = pl.ds(pl.multiple_of(t * tile, tile), tile)
        up_at = pl.ds(pl.multiple_of(hid + t * tile, tile), tile)
        d_hidden = dot(routed[...], dw[at, :], ((1,), (1,)))
        gate, up = pre[:, at], pre[:, up_at]
        sig = jax.nn.sigmoid(gate)
        act = gate * sig
        hidden[:, at] = (act * up).astype(BF)
        dall[:, at] = (d_hidden * up * sig * (1.0 + gate * (1.0 - sig))).astype(BF)
        dall[:, up_at] = (d_hidden * act).astype(BF)

    def back_part(block, place):
        @pl.loop(0, chan // tile)
        def _(t):
            at = pl.ds(pl.multiple_of(block * chan + t * tile, tile), tile)
            value = dot(dall[...], w[at, :], ((1,), (1,)))
            parts[place, :, pl.ds(pl.multiple_of(t * tile, tile), tile)] = value.astype(BF)

    far_sib = lax.rem(sib + n_tp // 2, n_tp)
    sib_copies = [
        remote(parts.at[2 * i], from_sib.at[i], sib_sems.at[0, i], sib_sems.at[1, i], {"tp": sib})
        for i in range(2)
    ]

    def at_rows(d):
        s = lax.rem(me + d, n_sp)
        return pl.ds(pl.multiple_of(s * cap, cap), cap)

    def far_copy(d):
        return remote(
            far_out.at[at_rows(d), :], far_in.at[at_rows(d), :],
            far_sems.at[0, lax.rem(d, n_sp)], far_sems.at[1, lax.rem(d, n_sp)], {"tp": far},
        )

    def ret_copy(d):
        mine = pl.ds(pl.multiple_of(me * cap, cap), cap)
        return remote(
            final.at[at_rows(d), :], back.at[mine, :],
            ret_sems.at[0, d], ret_sems.at[1, d], {"sp": lax.rem(me + d, n_sp)},
        )

    back_part(far_sib, 0)
    sib_copies[0].start()
    back_part(far, 1)
    sib_copies[0].wait_recv()

    @pl.loop(1, n_sp + 1)
    def _(d):
        at = at_rows(d)
        far_out[at, :] = (parts[1, at, :].astype(F32) + from_sib[0, at, :].astype(F32)).astype(BF)
        far_copy(d).start()

    back_part(sib, 2)
    sib_copies[1].start()
    back_part(tp, 3)
    sib_copies[1].wait_recv()
    total[...] = parts[3].astype(F32) + from_sib[1].astype(F32)

    @pl.loop(1, n_sp)
    def _(d):
        at = at_rows(d)
        far_copy(d).wait_recv()
        final[at, :] = (total[at, :] + far_in[at, :].astype(F32)).astype(BF)
        ret_copy(d).start()

    far_copy(n_sp).wait_recv()
    at = at_rows(0)
    back[at, :] = (total[at, :] + far_in[at, :].astype(F32)).astype(BF)

    @pl.loop(1, n_sp)
    def _(d):
        ret_copy(d).wait_recv()

    value = (og_ref[...].astype(F32) + dot(disp[...], back[...], ((1,), (0,)))).astype(BF)
    resid[...] = value
    rfull[tp] = value
    near = remote(rfull.at[tp], rfull.at[tp], gat_sems.at[0], gat_sems.at[1], {"tp": sib})
    away = remote(rfull.at[tp], rfull.at[tp], gat_sems.at[2], gat_sems.at[3], {"tp": far})
    away.start()
    near.start()
    away.wait_recv()
    hand = remote(rfull.at[far], rfull.at[far], gat_sems.at[4], gat_sems.at[5], {"tp": sib})
    hand.start()
    near.wait_recv()
    hand.wait_recv()
    share = tokens // n_tp
    piece = width // n_sp
    for k in range(n_sp):
        block, first = divmod(k * piece, chan)
        quarter[k] = rfull[
            block, pl.ds(pl.multiple_of(tp * share, share), share), first:first + piece
        ]
    near.wait_send()
    away.wait_send()
    hand.wait_send()
    for copy in sib_copies:
        copy.wait_send()

    @pl.loop(1, n_sp)
    def _(d):
        far_copy(d).wait_send()
        ret_copy(d).wait_send()

    far_copy(n_sp).wait_send()


def mixer_kernel(
    n_sp, n_tp,
    quarter, rfull, pw_hbm, og_ref, ig_ref, val_ref, conv_ref, taps_ref,
    columns, og_out, ig_out, val_out,
    pw, edge_out, edge_in, ex_sems, halo_sems, load_sem,
):
    me, tp = lax.axis_index("sp"), lax.axis_index("tp")
    sib = tp + 1 - 2 * lax.rem(tp, 2)
    far = lax.rem(tp + n_tp // 2, n_tp)
    tokens, chan = og_ref.shape
    load = pltpu.make_async_copy(pw_hbm, pw, load_sem)
    load.start()
    hail(n_sp, me, (sib, far))
    met(n_sp, (sib, far))
    ex = Exchange(
        n_sp, me, tp, sib, far, lambda k: quarter.at[k], lambda j, s: columns.at[s, j], ex_sems
    )
    ex.start()
    load.wait()
    mix = dot(rfull[0], pw[0:chan, :], ((1,), (0,)))
    for j in range(1, n_tp):
        mix = mix + dot(rfull[j], pw[j * chan:(j + 1) * chan, :], ((1,), (0,)))
    og_out[...] = (mix * conv_ref[...].astype(F32)).astype(BF)
    grad = (mix * og_ref[...].astype(F32)).astype(BF).astype(F32)
    edge_out[0] = jnp.broadcast_to(grad[tokens - 1:tokens, :], edge_out.shape[1:])
    edge_out[1] = jnp.broadcast_to(grad[0:1, :], edge_out.shape[1:])
    sides = [lax.rem(me + 1, n_sp), lax.rem(me + n_sp - 1, n_sp)]
    halos = [
        remote(edge_out.at[i], edge_in.at[i], halo_sems.at[0, i], halo_sems.at[1, i], {"sp": sides[i]})
        for i in range(2)
    ]
    for halo in halos:
        halo.start()
    pl.loop(1, n_sp)(ex.spread)
    pl.loop(0, n_sp)(ex.hand)
    for halo in halos:
        halo.wait()
    before = jnp.where(me == 0, 0.0, edge_in[0, 0:1, :])
    after = jnp.where(me == n_sp - 1, 0.0, edge_in[1, 0:1, :])
    row = lax.broadcasted_iota(jnp.int32, (tokens, chan), 0)
    prev = jnp.where(row == 0, before, pltpu.roll(grad, 1, 0))
    following = jnp.where(row == tokens - 1, after, pltpu.roll(grad, tokens - 1, 0))
    taps = taps_ref[...].astype(F32)
    value_grad = following * taps[0:1, :] + grad * taps[1:2, :] + prev * taps[2:3, :]
    ig_out[...] = (value_grad * val_ref[...].astype(F32)).astype(BF)
    val_out[...] = (value_grad * ig_ref[...].astype(F32)).astype(BF)
    ex.finish()


def in_grads(scale, x, d, gate, up):
    hid = gate.shape[-1]
    left = x[0].T
    gate[0] = (dot(left, d[:, :hid], ((1,), (0,))) * scale).astype(BF)
    up[0] = (dot(left, d[:, hid:], ((1,), (0,))) * scale).astype(BF)


def out_grads(scale, h, r, down):
    down[0] = (dot(h[...].T, r[...], ((1,), (0,))) * scale).astype(BF)


def per_device(
    out_grad, route_ids, route_weight, expert_inputs, gate_weight, up_weight, down_weight,
    out_gate, in_gate, values, conv_out, conv_taps, proj_weight,
):
    n_sp, n_tp = lax.axis_size("sp"), lax.axis_size("tp")
    tokens, chan = out_grad.shape
    local, slots, width = expert_inputs.shape
    hid = gate_weight.shape[2]
    assert local == 1 and n_tp == 4
    share, piece = tokens // n_tp, width // n_sp
    dma = pltpu.SemaphoreType.DMA
    mixed_in = (out_gate.astype(F32) * conv_out.astype(F32)).astype(BF)
    mixed_all = lax.all_gather(mixed_in, "sp", axis=0, tiled=True)

    routed, hidden, dall, resid, rfull, quarter = pl.pallas_call(
        functools.partial(expert_kernel, n_sp, n_tp, n_sp * local),
        out_shape=[
            jax.ShapeDtypeStruct((slots, width), BF),
            jax.ShapeDtypeStruct((slots, hid), BF),
            jax.ShapeDtypeStruct((slots, 2 * hid), BF),
            jax.ShapeDtypeStruct((tokens, chan), BF),
            jax.ShapeDtypeStruct((n_tp, tokens, chan), BF),
            jax.ShapeDtypeStruct((n_sp, share, piece), BF),
        ],
        in_specs=[VMEM] * 3 + [ANY] * 4,
        out_specs=[VMEM] * 6,
        scratch_shapes=[
            pltpu.VMEM((slots, width), BF),
            pltpu.VMEM((width, 2 * hid), BF),
            pltpu.VMEM((hid, width), BF),
            pltpu.VMEM((slots, 2 * hid), F32),
            pltpu.VMEM((slots, chan), BF),
            pltpu.VMEM((4, slots, chan), BF),
            pltpu.VMEM((2, slots, chan), BF),
            pltpu.VMEM((slots, chan), BF),
            pltpu.VMEM((slots, chan), BF),
            pltpu.VMEM((slots, chan), F32),
            pltpu.VMEM((slots, chan), BF),
            pltpu.VMEM((slots, chan), BF),
            pltpu.VMEM((tokens, slots), BF),
            dma((4,)), dma((8, n_sp)), dma((2, 2)), dma((2, n_sp)), dma((2, n_sp)), dma((6,)),
        ],
        compiler_params=pltpu.CompilerParams(
            collective_id=0, has_side_effects=True, vmem_limit_bytes=48 * 2**20
        ),
        name="experts",
    )(out_grad, route_ids, route_weight, expert_inputs, gate_weight, up_weight, down_weight)

    columns, out_gate_grad, in_gate_grad, values_grad = pl.pallas_call(
        functools.partial(mixer_kernel, n_sp, n_tp),
        out_shape=[
            jax.ShapeDtypeStruct((n_sp, n_tp, share, piece), BF),
            jax.ShapeDtypeStruct((tokens, chan), BF),
            jax.ShapeDtypeStruct((tokens, chan), BF),
            jax.ShapeDtypeStruct((tokens, chan), BF),
        ],
        in_specs=[VMEM, VMEM, ANY] + [VMEM] * 5,
        out_specs=[VMEM] * 4,
        scratch_shapes=[
            pltpu.VMEM(proj_weight.shape, BF),
            pltpu.VMEM((2, 8, chan), F32),
            pltpu.VMEM((2, 8, chan), F32),
            dma((8, n_sp)), dma((2, 2)), dma,
        ],
        compiler_params=pltpu.CompilerParams(
            collective_id=1, has_side_effects=True, vmem_limit_bytes=32 * 2**20
        ),
        name="mixer",
    )(quarter, rfull, proj_weight, out_gate, in_gate, values, conv_out, conv_taps)

    slot_scale = 1.0 / math.sqrt(slots)
    wide = 512
    gate_grad, up_grad = pl.pallas_call(
        functools.partial(in_grads, slot_scale),
        grid=(width // wide,),
        in_specs=[
            pl.BlockSpec((1, slots, wide), lambda i: (0, 0, i)),
            pl.BlockSpec((slots, 2 * hid), lambda i: (0, 0)),
        ],
        out_specs=[pl.BlockSpec((1, wide, hid), lambda i: (0, i, 0))] * 2,
        out_shape=[jax.ShapeDtypeStruct((1, width, hid), BF)] * 2,
        name="in_grads",
    )(expert_inputs, dall)
    down_grad = pl.pallas_call(
        functools.partial(out_grads, slot_scale),
        grid=(hid // 256,),
        in_specs=[
            pl.BlockSpec((slots, 256), lambda i: (0, i)),
            pl.BlockSpec((slots, width), lambda i: (0, 0)),
        ],
        out_specs=pl.BlockSpec((1, 256, width), lambda i: (0, i, 0)),
        out_shape=jax.ShapeDtypeStruct((1, hid, width), BF),
        name="out_grads",
    )(hidden, routed)
    proj_sum = lax.dot_general(
        columns.reshape(n_sp * tokens, piece), mixed_all,
        (((0,), (0,)), ((), ())), preferred_element_type=F32,
    )
    proj_grad = proj_sum * (1.0 / math.sqrt(tokens * n_sp))
    return (
        resid, out_gate_grad, in_gate_grad, values_grad, proj_grad, gate_grad, up_grad, down_grad,
    )


def solution(mesh):
    rows = P("sp", "tp")
    in_specs = (
        rows, P("sp", None), P("sp", None), P("sp", None, None), P("sp", None, "tp"),
        P("sp", None, "tp"), P("sp", "tp", None), rows, rows, rows, rows, P(None, "tp"), P(None, "tp"),
    )
    out_specs = (
        rows, rows, rows, rows, rows, P("sp", None, "tp"), P("sp", None, "tp"), P("sp", "tp", None),
    )
    return jax.shard_map(
        per_device, mesh=mesh, in_specs=in_specs, out_specs=out_specs, check_vma=False
    )
```
